32 devices in a mesh: sp: 16 (over z, y, x), tp: 2 (over core).
Axes of the slice: x: 2, y: 2, z: 4, core: 2. Of those that a mesh axis runs over, the one named last changes fastest.
Arguments:
- mid_stream: bfloat16 [5120, 2048], P('sp', 'tp'), may hold values from -6 to 6
- layer_cot: bfloat16 [5120, 2048], P('sp', 'tp'), may hold values from -6 to 6
- ffn_gain: bfloat16 [2048], P('tp'), may hold values from 0.099609375 to 1.8984375
- expert_ids: int32 [5120, 2], P('sp'), may hold values from 0 to 15, all different within a row; in each aligned block of 320 rows (0 to 319, 320 to 639, ...) at most 80 rows name the same one
- group_prob: float32 [5120], P('sp'), may hold values from 0.25 to 1
- first_share: float32 [5120], P('sp'), may hold values from 0.5 to 0.95
- expert_gate: bfloat16 [16, 2048, 1024], P('sp', None, 'tp'), may hold values from -0.125 to 0.125
- expert_up: bfloat16 [16, 2048, 1024], P('sp', None, 'tp'), may hold values from -0.125 to 0.125
- expert_down: bfloat16 [16, 1024, 2048], P('sp', 'tp'), may hold values from -0.1875 to 0.1875
- out_weight: bfloat16 [2048, 1024], P(None, 'tp'), may hold values from -0.1875 to 0.1875
- conv_gain: bfloat16 [1024], P('tp'), may hold values from 0.099609375 to 1.8984375
- b_gate: bfloat16 [5120, 1024], P('sp', 'tp'), may hold values from -6 to 6
- c_gate: bfloat16 [5120, 1024], P('sp', 'tp'), may hold values from -6 to 6
- conv_in: bfloat16 [5120, 1024], P('sp', 'tp'), may hold values from -6 to 6
- conv_out: bfloat16 [5120, 1024], P('sp', 'tp'), may hold values from -6 to 6
- conv_taps: bfloat16 [3, 1024], P(None, 'tp'), may hold values from -3.5 to 3.5
Outputs:
- grad_gate: float32 [16, 2048, 1024], P('sp', None, 'tp')
- grad_up: float32 [16, 2048, 1024], P('sp', None, 'tp')
- grad_down: float32 [16, 1024, 2048], P('sp', 'tp')
- grad_out_weight: float32 [2048, 1024], P('sp', 'tp')
- mid_grad: bfloat16 [5120, 2048], P('sp', 'tp')
- grad_b: bfloat16 [5120, 1024], P('sp', 'tp')
- grad_c: bfloat16 [5120, 1024], P('sp', 'tp')
- grad_conv_in: bfloat16 [5120, 1024], P('sp', 'tp')
The draws below stay inside these ranges and needn't reach their ends.
Inputs may be any that keep to these rules, and one draw needn't show every extreme that they name: `expert_ids`: each row names 2 different experts. Among the rows of one device no expert is named more than 80 times, a bound that some block reaches.
All inputs are finite; a program needn't handle non-finite values.
Results may differ from the reference program's by a relative error of at most 0.0067.
Values may be sent and summed in bfloat16 or wider, within the bound.
No kernel may reach another device: no remote copies, remote signals or barrier semaphores. Data moves between devices by JAX's collectives and lax.ppermute only.
A program may use at most 128 MiB of HBM per device.

```python
import math
import jax
import jax.numpy as jnp
import numpy as np
from jax import lax

D = 2048
CONV_CH = 1024
GROUP = 64
FF = 1024
TOP = 2
TOK_DEV = 320
TOKENS = 5120
EXPERTS = 16
CAP = 80
N_SP = 16
N_TP = 2


def with_spikes(entries, key, source, target, parts, factor):
    def block_of(position):
        return (jnp.arange(entries.shape[position]) // (entries.shape[position] // parts)).reshape((-1,) + (1,) * (entries.ndim - 1 - position))

    first = jax.random.permutation(key, parts)[block_of(target)]
    far = (block_of(target) + parts // 2) % parts
    return jnp.where((block_of(source) == first) | (block_of(source) == far), factor * entries, entries)


def block_scale(rng, dims, shards, least, high):
    gain, own = 1.0, jax.random.fold_in(rng, 6)
    for dim, blocks in shards:
        draws = jnp.exp(jax.random.uniform(jax.random.fold_in(own, dim), (blocks,), jnp.float32, least / len(shards), high / len(shards)))
        gain = gain * jnp.repeat(draws, dims[dim] // blocks).reshape([-1 if axis == dim else 1 for axis in range(len(dims))])
    return gain


def shared_out(stream_key, own, number, rows, number_of, top, limit, skew):
    order = jax.random.permutation(stream_key, number_of)
    crowded, ordinary = portions_of(number_of, rows * top, limit, skew, True), portions_of(number_of, rows * top, limit, skew, False)
    places = jnp.arange(number_of)

    def named(lengths, offset_by):
        used = int((lengths > 0).sum())
        fixed = max(1, used // 4)
        moved = fixed + (places - fixed + offset_by * (used - fixed)) % max(1, number_of - fixed)
        return jnp.zeros((number_of,), jnp.int32).at[order[jnp.where(places < fixed, places, moved)]].set(jnp.asarray(lengths, jnp.int32))

    lengths = jnp.where(number % 4 == 0, named(crowded, number // 4), named(ordinary, number - number // 4 - 1))
    mixed = jax.random.permutation(jax.random.fold_in(own, 3), number_of)
    source_of, taker = mixed[0:number_of // 2 * 2:2], mixed[1:number_of // 2 * 2:2]
    slack = jnp.minimum(lengths[source_of] - 1, limit - lengths[taker]) // 2
    slack = jnp.where((source_of == order[0]) | (taker == order[0]) | (lengths[taker] == 0), 0, jnp.maximum(slack, 0))
    moved = jax.random.randint(jax.random.fold_in(own, 4), (number_of // 2,), 0, 1 << 20) % (slack + 1)
    lengths = lengths.at[source_of].add(-moved).at[taker].add(moved)
    items = jnp.searchsorted(jnp.cumsum(lengths), jnp.arange(rows * top), side="right").astype(jnp.int32)
    table = items.reshape(top, rows).T
    table = table[jax.random.permutation(jax.random.fold_in(own, 1), rows)]
    offset_by = jax.random.randint(jax.random.fold_in(own, 2), (rows, 1), 0, top)
    return jnp.take_along_axis(table, (jnp.arange(top)[None, :] + offset_by) % top, axis=1)


def portions_of(amount, total, limit, skew, full):
    loads = [(1 << 20) // math.isqrt(rank ** skew) + 1 for rank in range(1, amount + 1)]
    largest = limit if full else min(limit, max(-(-total // amount), total * loads[0] // sum(loads)))
    least = 1 if total - largest >= amount - 1 else 0
    given, rest = [largest] + [least] * (amount - 1), total - largest - least * (amount - 1)
    while rest > 0:
        free = [i for i in range(1, amount) if given[i] < largest] or [i for i in range(1, amount) if given[i] < limit]
        pool, remaining = sum([loads[i] for i in free]), rest
        for i in free:
            addition = min(limit - given[i], max(1, remaining * loads[i] // pool), rest)
            given[i] = given[i] + addition
            rest = rest - addition
    return np.array(given)


def bell_draw(key, extent, width, limit, shards=(), held_as=jnp.bfloat16):
    values = width * jax.random.normal(key, extent, jnp.float32)
    if shards:
        values = values * block_scale(key, extent, shards, -0.22, 0.18)
    return jnp.clip(values, -limit, limit).astype(held_as)


def bell_draw_with(stream_key, shape, scale, reach, cuts, heavy, kind=jnp.bfloat16):
    result = scale * jax.random.normal(stream_key, shape, jnp.float32)
    if cuts:
        result = result * block_scale(stream_key, shape, cuts, -0.22, 0.18)
    return jnp.clip(with_spikes(result, jax.random.fold_in(stream_key, 3), *heavy), -reach, reach).astype(kind)


def setup_inputs(seed: int = 0) -> dict:
    key_of = jax.random.split(jax.random.key(seed), 17)
    mid_stream = bell_draw(key_of[0], (TOKENS, D), 1.0, 6.0, ((0, 16), (1, 2)))
    layer_cot = bell_draw_with(key_of[1], (TOKENS, D), 1.0, 6.0, ((0, 16), (1, 2)), (0, 1, 16, 2.0))
    ffn_gain = jnp.clip(1.0 + 0.18 * jax.random.normal(key_of[2], (D,), jnp.float32), 0.099609375, 1.8984375).astype(jnp.bfloat16)
    expert_ids_keys = jax.random.split(jax.random.fold_in(key_of[3], 1), TOKENS // TOK_DEV)
    expert_ids_turns = jax.random.permutation(jax.random.fold_in(key_of[3], 3), TOKENS // TOK_DEV)
    expert_ids = jax.vmap(lambda own, number: shared_out(jax.random.fold_in(key_of[3], 2), own, number, TOK_DEV, EXPERTS, TOP, CAP, 2))(expert_ids_keys, expert_ids_turns).reshape((TOKENS, TOP))
    group_prob = jnp.clip(0.25 + 0.75 * jax.random.uniform(key_of[4], (TOKENS,), jnp.float32) ** block_scale(key_of[4], (TOKENS,), ((0, 16),), -0.2, 0.2), 0.25, 1.0)
    first_share = jnp.clip(0.5 + 0.45 * jax.random.uniform(key_of[5], (TOKENS,), jnp.float32) ** block_scale(key_of[5], (TOKENS,), ((0, 16),), -0.2, 0.2), 0.5, 0.95)
    expert_gate = bell_draw(key_of[6], (EXPERTS, D, FF), D ** -0.5, 0.125, ((0, 16), (2, 2)))
    expert_up = bell_draw(key_of[7], (EXPERTS, D, FF), D ** -0.5, 0.125, ((0, 16), (2, 2)))
    expert_down = bell_draw(key_of[8], (EXPERTS, FF, D), FF ** -0.5, 0.1875, ((0, 16), (1, 2)))
    out_weight = bell_draw(key_of[9], (D, CONV_CH), CONV_CH ** -0.5, 0.1875, ((1, 2),))
    conv_gain = jnp.clip(1.0 + 0.18 * jax.random.normal(key_of[10], (CONV_CH,), jnp.float32), 0.099609375, 1.8984375).astype(jnp.bfloat16)
    b_gate = bell_draw(key_of[11], (TOKENS, CONV_CH), 1.0, 6.0, ((0, 16), (1, 2)))
    c_gate = bell_draw(key_of[12], (TOKENS, CONV_CH), 1.0, 6.0, ((0, 16), (1, 2)))
    conv_in = bell_draw(key_of[13], (TOKENS, CONV_CH), 1.0, 6.0, ((0, 16), (1, 2)))
    conv_out = bell_draw(key_of[14], (TOKENS, CONV_CH), 1.0, 6.0, ((0, 16), (1, 2)))
    conv_taps = bell_draw(key_of[15], (3, CONV_CH), 3 ** -0.5, 3.5, ((1, 2),))
    return dict(mid_stream=mid_stream, layer_cot=layer_cot, ffn_gain=ffn_gain, expert_ids=expert_ids, group_prob=group_prob, first_share=first_share, expert_gate=expert_gate, expert_up=expert_up, expert_down=expert_down, out_weight=out_weight, conv_gain=conv_gain, b_gate=b_gate, c_gate=c_gate, conv_in=conv_in, conv_out=conv_out, conv_taps=conv_taps)


epsilon = 1e-06

def silu_parts(pre):
    sigma = jax.nn.sigmoid(pre)
    return (pre * sigma, sigma * (1.0 + pre * (1.0 - sigma)))

def expert_backward(tokens_in, cots_in, gate_w, up_w, down_w):
    pre_gate = jnp.dot(tokens_in, gate_w, preferred_element_type=jnp.float32)
    pre_up = jnp.dot(tokens_in, up_w, preferred_element_type=jnp.float32)
    active, slope = silu_parts(pre_gate)
    hidden = (active * pre_up).astype(jnp.bfloat16)
    grad_down = jnp.dot(hidden.T, cots_in, preferred_element_type=jnp.float32)
    d_hidden = jnp.dot(cots_in, down_w.T, preferred_element_type=jnp.float32)
    d_gate = (d_hidden * pre_up * slope).astype(jnp.bfloat16)
    d_up = (d_hidden * active).astype(jnp.bfloat16)
    grad_gate = jnp.dot(tokens_in.T, d_gate, preferred_element_type=jnp.float32)
    grad_up = jnp.dot(tokens_in.T, d_up, preferred_element_type=jnp.float32)
    block_width = FF // N_TP
    summed = jnp.zeros((tokens_in.shape[0], D), jnp.float32)
    for block_number in range(N_TP):
        first_col = block_number * block_width
        last_col = first_col + block_width
        partial_term = jnp.dot(d_gate[:, first_col:last_col], gate_w[:, first_col:last_col].T, preferred_element_type=jnp.float32)
        partial_term = partial_term + jnp.dot(d_up[:, first_col:last_col], up_w[:, first_col:last_col].T, preferred_element_type=jnp.float32)
        rounded = lax.optimization_barrier(partial_term.astype(jnp.bfloat16))
        summed = summed + rounded.astype(jnp.float32)
    return (grad_gate, grad_up, grad_down, summed.astype(jnp.bfloat16))

def reference(mid_stream, layer_cot, ffn_gain, expert_ids, group_prob, first_share, expert_gate, expert_up, expert_down, out_weight, conv_gain, b_gate, c_gate, conv_in, conv_out, conv_taps):
    token_count = mid_stream.shape[0]
    mid32 = mid_stream.astype(jnp.float32)
    gain32 = ffn_gain.astype(jnp.float32)
    inv_rms = lax.rsqrt(lax.optimization_barrier(jnp.mean(mid32 * mid32, axis=1)) + epsilon)
    normed = (mid32 * inv_rms[:, None] * gain32).astype(jnp.bfloat16)
    shares = jnp.stack([group_prob * first_share, group_prob * (1.0 - first_share)], axis=1)
    weighted = (layer_cot.astype(jnp.float32)[:, None, :] * shares[:, :, None]).astype(jnp.bfloat16)
    flat_ids = expert_ids.reshape(-1).astype(jnp.int32)
    pair_count = flat_ids.shape[0]
    depth = N_SP * CAP
    onehot = (flat_ids[:, None] == jnp.arange(EXPERTS, dtype=jnp.int32)[None, :]).astype(jnp.int32)
    before = jnp.cumsum(onehot, axis=0) - onehot
    ranks = lax.optimization_barrier(jnp.sum(before * onehot, axis=1)).astype(jnp.int32)
    slot_index = (flat_ids * depth + ranks).astype(jnp.int32)
    source = jnp.full((EXPERTS * depth,), pair_count, jnp.int32)
    source = source.at[slot_index].set(jnp.arange(pair_count, dtype=jnp.int32)).reshape(EXPERTS, depth)
    normed_pad = jnp.concatenate([normed, jnp.zeros((1, D), jnp.bfloat16)], axis=0)
    weighted_pad = jnp.concatenate([weighted.reshape(pair_count, D), jnp.zeros((1, D), jnp.bfloat16)], axis=0)

    def per_expert(packed):
        rows_of, gate_w, up_w, down_w = packed
        tokens_in = normed_pad[rows_of // 2]
        cots_in = weighted_pad[rows_of]
        return expert_backward(tokens_in, cots_in, gate_w, up_w, down_w)
    grad_gate, grad_up, grad_down, back_all = lax.map(per_expert, (source, expert_gate, expert_up, expert_down))
    back_rows = back_all.reshape(EXPERTS * depth, D)[slot_index]
    d_normed = lax.optimization_barrier(jnp.sum(back_rows.astype(jnp.float32).reshape(token_count, TOP, D), axis=1))
    g_dn = gain32 * d_normed
    inner = lax.optimization_barrier(jnp.mean(mid32 * g_dn, axis=1))
    mid_total = layer_cot.astype(jnp.float32) + inv_rms[:, None] * g_dn - mid32 * (inv_rms ** 3 * inner)[:, None]
    mid_grad = mid_total.astype(jnp.bfloat16)
    b32 = b_gate.astype(jnp.float32)
    y32 = conv_out.astype(jnp.float32)
    grouped = (b32 * y32).reshape(token_count, CONV_CH // GROUP, GROUP)
    group_rms = lax.rsqrt(lax.optimization_barrier(jnp.mean(grouped * grouped, axis=-1)) + epsilon)
    cgain = conv_gain.astype(jnp.float32).reshape(CONV_CH // GROUP, GROUP)
    conv_normed = (grouped * group_rms[..., None] * cgain).reshape(token_count, CONV_CH).astype(jnp.bfloat16)
    grad_out_weight = jnp.dot(mid_grad.T, conv_normed, preferred_element_type=jnp.float32)
    d_normed_conv = jnp.dot(mid_grad, out_weight, preferred_element_type=jnp.float32).reshape(grouped.shape)
    g_dc = cgain * d_normed_conv
    group_inner = lax.optimization_barrier(jnp.mean(grouped * g_dc, axis=-1))
    d_gated = (group_rms[..., None] * g_dc - grouped * (group_rms ** 3 * group_inner)[..., None]).reshape(token_count, CONV_CH)
    grad_b = (d_gated * y32).astype(jnp.bfloat16)
    d_conv_out = d_gated * b32
    extended = jnp.concatenate([d_conv_out, jnp.zeros((2, CONV_CH), jnp.float32)], axis=0)
    taps = conv_taps.astype(jnp.float32)
    d_mixed = taps[2] * extended[:-2] + taps[1] * extended[1:-1] + taps[0] * extended[2:]
    grad_c = (d_mixed * conv_in.astype(jnp.float32)).astype(jnp.bfloat16)
    grad_conv_in = (d_mixed * c_gate.astype(jnp.float32)).astype(jnp.bfloat16)
    return (grad_gate, grad_up, grad_down, grad_out_weight, mid_grad, grad_b, grad_c, grad_conv_in)
```

```python
import jax
import jax.numpy as jnp
from jax import lax
from jax.sharding import PartitionSpec as P

D = 2048
GROUP = 64


epsilon = 1e-06


def from_behind(block, axis, distance):
    devices = range(lax.axis_size(axis))
    route = [(i - distance, i) for i in devices if i - distance in devices]
    return lax.ppermute(block, axis, route)


def swap_pair(block):
    return lax.ppermute(block, "tp", [(0, 1), (1, 0)])


def join_pair(block, axis):
    other = swap_pair(block)
    first = lax.axis_index("tp") == 0
    low = jnp.where(first, block, other)
    high = jnp.where(first, other, block)
    return jnp.concatenate([low, high], axis=axis)


def scatter_sum(partial):
    device_count = lax.axis_size("sp")
    inner = 1
    while inner * inner < device_count:
        inner *= 2
    outer = device_count // inner
    near = [[o * inner + k for k in range(inner)] for o in range(outer)]
    far = [[o * inner + k for o in range(outer)] for k in range(inner)]
    rows = partial.shape[0] // device_count
    cols = partial.shape[1]
    blocks = partial.astype(jnp.bfloat16).reshape(outer, inner, rows, cols).transpose(1, 0, 2, 3)
    moved = lax.all_to_all(blocks, "sp", 0, 0, tiled=True, axis_index_groups=near)
    part = jnp.sum(moved.astype(jnp.float32), axis=0).astype(jnp.bfloat16)
    moved = lax.all_to_all(part, "sp", 0, 0, tiled=True, axis_index_groups=far)
    return jnp.sum(moved.astype(jnp.float32), axis=0)


def silu_parts(pre):
    sigma = jax.nn.sigmoid(pre)
    return (pre * sigma, sigma * (1.0 + pre * (1.0 - sigma)))


def contract_rows(left, right):
    return lax.dot_general(
        left, right, (((0,), (0,)), ((), ())), preferred_element_type=jnp.float32
    )


def contract_cols(left, right):
    return lax.dot_general(
        left, right, (((1,), (1,)), ((), ())), preferred_element_type=jnp.float32
    )


def expert_pass(token_rows, cot_rows, expert_gate, expert_up, expert_down):
    moved_tokens = lax.all_to_all(token_rows, "sp", split_axis=0, concat_axis=0, tiled=True)
    moved_cots = lax.all_to_all(cot_rows, "sp", split_axis=0, concat_axis=0, tiled=True)
    full_tokens = join_pair(moved_tokens, 2)
    local_count = expert_gate.shape[0]
    source_count = full_tokens.shape[0] // local_count
    slot_count = full_tokens.shape[1]
    split_tokens = full_tokens.reshape(source_count, local_count, slot_count, D)
    tokens_in = split_tokens[:, 0].reshape(source_count * slot_count, D)
    gate_w = expert_gate[0]
    up_w = expert_up[0]
    pre_gate = jnp.dot(tokens_in, gate_w, preferred_element_type=jnp.float32)
    pre_up = jnp.dot(tokens_in, up_w, preferred_element_type=jnp.float32)
    pre_gate, pre_up, moved_cots = lax.optimization_barrier((pre_gate, pre_up, moved_cots))
    full_cots = join_pair(moved_cots, 2)
    split_cots = full_cots.reshape(source_count, local_count, slot_count, D)
    cots_in = split_cots[:, 0].reshape(source_count * slot_count, D)
    active, slope = silu_parts(pre_gate)
    hidden = (active * pre_up).astype(jnp.bfloat16)
    down_grads = [contract_rows(hidden, cots_in)]
    d_hidden = contract_cols(cots_in, expert_down[0])
    d_gate = (d_hidden * pre_up * slope).astype(jnp.bfloat16)
    d_up = (d_hidden * active).astype(jnp.bfloat16)
    gate_grads = [contract_rows(tokens_in, d_gate)]
    up_grads = [contract_rows(tokens_in, d_up)]
    half = D // 2
    mine = lax.axis_index("tp") * half

    def term(start):
        gate_part = lax.dynamic_slice_in_dim(gate_w, start, half, axis=0)
        up_part = lax.dynamic_slice_in_dim(up_w, start, half, axis=0)
        product = contract_cols(d_gate, gate_part) + contract_cols(d_up, up_part)
        return product.astype(jnp.bfloat16)

    received = swap_pair(term(half - mine))
    summed = (term(mine).astype(jnp.float32) + received.astype(jnp.float32)).astype(jnp.bfloat16)
    summed = summed.reshape(source_count * local_count, slot_count, half)
    returned = lax.all_to_all(summed, "sp", split_axis=0, concat_axis=0, tiled=True)
    grads = (
        jnp.stack(gate_grads, axis=0),
        jnp.stack(up_grads, axis=0),
        jnp.stack(down_grads, axis=0),
    )
    return lax.optimization_barrier((returned, grads))


def shards(
    mid_stream,
    layer_cot,
    ffn_gain,
    expert_ids,
    group_prob,
    first_share,
    expert_gate,
    expert_up,
    expert_down,
    out_weight,
    conv_gain,
    b_gate,
    c_gate,
    conv_in,
    conv_out,
    conv_taps,
):
    row_count = mid_stream.shape[0]
    half_width = mid_stream.shape[1]
    expert_count = lax.axis_size("sp") * expert_gate.shape[0]
    slot_count = 4 * row_count // expert_count
    mid32 = mid_stream.astype(jnp.float32)
    gain32 = ffn_gain.astype(jnp.float32)
    square_sum = lax.psum(jnp.sum(mid32 * mid32, axis=1), "tp")
    inv_rms = lax.rsqrt(square_sum / D + epsilon)
    normed = (mid32 * inv_rms[:, None] * gain32).astype(jnp.bfloat16)
    shares = jnp.stack([group_prob * first_share, group_prob * (1.0 - first_share)], axis=1)
    flat_ids = expert_ids.reshape(-1)
    pair_count = flat_ids.shape[0]
    onehot = (flat_ids[:, None] == jnp.arange(expert_count, dtype=jnp.int32)[None, :]).astype(
        jnp.int32
    )
    before = jnp.cumsum(onehot, axis=0) - onehot
    ranks = jnp.sum(before * onehot, axis=1)
    slot_index = flat_ids * slot_count + ranks
    source = jnp.full((expert_count * slot_count,), pair_count, jnp.int32)
    source = source.at[slot_index].set(jnp.arange(pair_count, dtype=jnp.int32))
    normed_pad = jnp.concatenate([normed, jnp.zeros((1, half_width), jnp.bfloat16)], axis=0)
    cot_pad = jnp.concatenate([layer_cot, jnp.zeros((1, half_width), jnp.bfloat16)], axis=0)
    share_pad = jnp.concatenate([shares.reshape(-1), jnp.zeros((2,), jnp.float32)])
    token_rows = normed_pad[source // 2].reshape(expert_count, slot_count, half_width)
    cot_rows = (cot_pad[source // 2].astype(jnp.float32) * share_pad[source][:, None]).astype(
        jnp.bfloat16
    )
    cot_rows = cot_rows.reshape(expert_count, slot_count, half_width)
    back_rows, grads = expert_pass(token_rows, cot_rows, expert_gate, expert_up, expert_down)
    flat_back = back_rows.reshape(expert_count * slot_count, half_width)
    slots = slot_index.reshape(row_count, 2)
    d_normed = flat_back[slots[:, 0]].astype(jnp.float32) + flat_back[slots[:, 1]].astype(jnp.float32)
    g_dn = gain32 * d_normed
    inner = lax.psum(jnp.sum(mid32 * g_dn, axis=1), "tp") / D
    mid_total = (
        layer_cot.astype(jnp.float32)
        + inv_rms[:, None] * g_dn
        - mid32 * (inv_rms**3 * inner)[:, None]
    )
    mid_grad = mid_total.astype(jnp.bfloat16)
    full_mid = join_pair(mid_grad, 1)
    channel_count = b_gate.shape[1]
    b32 = b_gate.astype(jnp.float32)
    y32 = conv_out.astype(jnp.float32)
    grouped = (b32 * y32).reshape(row_count, channel_count // GROUP, GROUP)
    group_rms = lax.rsqrt(jnp.mean(grouped * grouped, axis=-1) + epsilon)
    cgain = conv_gain.astype(jnp.float32).reshape(channel_count // GROUP, GROUP)
    conv_normed = (
        (grouped * group_rms[..., None] * cgain)
        .reshape(row_count, channel_count)
        .astype(jnp.bfloat16)
    )
    grad_out_weight = scatter_sum(contract_rows(full_mid, conv_normed))
    d_normed_conv = jnp.dot(full_mid, out_weight, preferred_element_type=jnp.float32).reshape(
        grouped.shape
    )
    g_dc = cgain * d_normed_conv
    group_inner = jnp.mean(grouped * g_dc, axis=-1)
    d_gated = (
        group_rms[..., None] * g_dc - grouped * (group_rms**3 * group_inner)[..., None]
    ).reshape(row_count, channel_count)
    grad_b = (d_gated * y32).astype(jnp.bfloat16)
    d_conv_out = d_gated * b32
    following = from_behind(d_conv_out[:2], "sp", -1)
    extended = jnp.concatenate([d_conv_out, following], axis=0)
    taps = conv_taps.astype(jnp.float32)
    d_mixed = taps[2] * extended[:-2] + taps[1] * extended[1:-1] + taps[0] * extended[2:]
    grad_c = (d_mixed * conv_in.astype(jnp.float32)).astype(jnp.bfloat16)
    grad_conv_in = (d_mixed * c_gate.astype(jnp.float32)).astype(jnp.bfloat16)
    return (grads[0], grads[1], grads[2], grad_out_weight, mid_grad, grad_b, grad_c, grad_conv_in)


def solution(mesh):
    placed = (
        P("sp", "tp"),
        P("sp", "tp"),
        P("tp"),
        P("sp", None),
        P("sp"),
        P("sp"),
        P("sp", None, "tp"),
        P("sp", None, "tp"),
        P("sp", "tp", None),
        P(None, "tp"),
        P("tp"),
        P("sp", "tp"),
        P("sp", "tp"),
        P("sp", "tp"),
        P("sp", "tp"),
        P(None, "tp"),
    )
    return jax.shard_map(
        shards,
        mesh=mesh,
        in_specs=placed,
        out_specs=(
            P("sp", None, "tp"),
            P("sp", None, "tp"),
            P("sp", "tp", None),
            P("sp", "tp"),
            P("sp", "tp"),
            P("sp", "tp"),
            P("sp", "tp"),
            P("sp", "tp"),
        ),
        check_vma=False,
    )
```

```python
import jax
import jax.numpy as jnp
from jax import lax
from jax.sharding import PartitionSpec as P

D = 2048
GROUP = 64


epsilon = 1e-06


def from_behind(block, axis, distance):
    devices = range(lax.axis_size(axis))
    route = [(i - distance, i) for i in devices if i - distance in devices]
    return lax.ppermute(block, axis, route)


def swap_pair(block):
    return lax.ppermute(block, "tp", [(0, 1), (1, 0)])


def swap_half(block):
    device_count = lax.axis_size("sp")
    half = device_count // 2
    return lax.ppermute(block, "sp", [(i, (i + half) % device_count) for i in range(device_count)])


def within_half(rows):
    half = lax.axis_size("sp") // 2
    groups = [[h * half + i for i in range(half)] for h in range(2)]
    return lax.all_to_all(rows, "sp", 0, 0, tiled=True, axis_index_groups=groups)


def join_pair(block, axis):
    other = swap_pair(block)
    first = lax.axis_index("tp") == 0
    low = jnp.where(first, block, other)
    high = jnp.where(first, other, block)
    return jnp.concatenate([low, high], axis=axis)


def scatter_sum(partial):
    device_count = lax.axis_size("sp")
    inner = 1
    while inner * inner < device_count:
        inner *= 2
    outer = device_count // inner
    near = [[o * inner + k for k in range(inner)] for o in range(outer)]
    far = [[o * inner + k for o in range(outer)] for k in range(inner)]
    rows = partial.shape[0] // device_count
    cols = partial.shape[1]
    blocks = partial.astype(jnp.bfloat16).reshape(outer, inner, rows, cols).transpose(1, 0, 2, 3)
    moved = lax.all_to_all(blocks, "sp", 0, 0, tiled=True, axis_index_groups=near)
    part = jnp.sum(moved.astype(jnp.float32), axis=0).astype(jnp.bfloat16)
    moved = lax.all_to_all(part, "sp", 0, 0, tiled=True, axis_index_groups=far)
    return jnp.sum(moved.astype(jnp.float32), axis=0)


def silu_parts(pre):
    sigma = jax.nn.sigmoid(pre)
    return (pre * sigma, sigma * (1.0 + pre * (1.0 - sigma)))


def contract_rows(left, right):
    return lax.dot_general(
        left, right, (((0,), (0,)), ((), ())), preferred_element_type=jnp.float32
    )


def contract_cols(left, right):
    return lax.dot_general(
        left, right, (((1,), (1,)), ((), ())), preferred_element_type=jnp.float32
    )


def expert_pass(token_rows, cot_rows, expert_gate, expert_up, expert_down):
    moved_tokens = within_half(token_rows)
    moved_cots = within_half(cot_rows)
    full_tokens = join_pair(moved_tokens, 2)
    local_count = expert_gate.shape[0]
    source_count = full_tokens.shape[0] // local_count
    slot_count = full_tokens.shape[1]
    split_tokens = full_tokens.reshape(source_count, local_count, slot_count, D)
    tokens_in = split_tokens[:, 0].reshape(source_count * slot_count, D)
    gate_w = expert_gate[0]
    up_w = expert_up[0]
    pre_gate = jnp.dot(tokens_in, gate_w, preferred_element_type=jnp.float32)
    pre_up = jnp.dot(tokens_in, up_w, preferred_element_type=jnp.float32)
    pre_gate, pre_up, moved_cots = lax.optimization_barrier((pre_gate, pre_up, moved_cots))
    full_cots = join_pair(moved_cots, 2)
    split_cots = full_cots.reshape(source_count, local_count, slot_count, D)
    cots_in = split_cots[:, 0].reshape(source_count * slot_count, D)
    active, slope = silu_parts(pre_gate)
    hidden = (active * pre_up).astype(jnp.bfloat16)
    down_grads = [contract_rows(hidden, cots_in)]
    d_hidden = contract_cols(cots_in, expert_down[0])
    d_gate = (d_hidden * pre_up * slope).astype(jnp.bfloat16)
    d_up = (d_hidden * active).astype(jnp.bfloat16)
    gate_grads = [contract_rows(tokens_in, d_gate)]
    up_grads = [contract_rows(tokens_in, d_up)]
    half = D // 2
    mine = lax.axis_index("tp") * half

    def term(start):
        gate_part = lax.dynamic_slice_in_dim(gate_w, start, half, axis=0)
        up_part = lax.dynamic_slice_in_dim(up_w, start, half, axis=0)
        product = contract_cols(d_gate, gate_part) + contract_cols(d_up, up_part)
        return product.astype(jnp.bfloat16)

    received = swap_pair(term(half - mine))
    summed = (term(mine).astype(jnp.float32) + received.astype(jnp.float32)).astype(jnp.bfloat16)
    summed = summed.reshape(source_count, 2, slot_count // 2, half).transpose(1, 0, 2, 3)
    summed = summed.reshape(2 * source_count, slot_count // 2, half)
    returned = lax.all_to_all(summed, "sp", split_axis=0, concat_axis=0, tiled=True)
    grads = (
        jnp.stack(gate_grads, axis=0),
        jnp.stack(up_grads, axis=0),
        jnp.stack(down_grads, axis=0),
    )
    return lax.optimization_barrier((returned, grads))


def shards(
    mid_stream,
    layer_cot,
    ffn_gain,
    expert_ids,
    group_prob,
    first_share,
    expert_gate,
    expert_up,
    expert_down,
    out_weight,
    conv_gain,
    b_gate,
    c_gate,
    conv_in,
    conv_out,
    conv_taps,
):
    row_count = mid_stream.shape[0]
    half_width = mid_stream.shape[1]
    expert_count = lax.axis_size("sp") * expert_gate.shape[0]
    slot_count = 4 * row_count // expert_count
    mid32 = mid_stream.astype(jnp.float32)
    gain32 = ffn_gain.astype(jnp.float32)
    square_sum = lax.psum(jnp.sum(mid32 * mid32, axis=1), "tp")
    inv_rms = lax.rsqrt(square_sum / D + epsilon)
    normed = (mid32 * inv_rms[:, None] * gain32).astype(jnp.bfloat16)
    shares = jnp.stack([group_prob * first_share, group_prob * (1.0 - first_share)], axis=1)
    half_count = expert_count // 2
    my_half = lax.axis_index("sp") // (lax.axis_size("sp") // 2)
    both_ids = jnp.stack([expert_ids.reshape(-1), swap_half(expert_ids).reshape(-1)])
    both_shares = jnp.concatenate([shares, swap_half(shares)]).reshape(-1)
    pair_count = both_ids.shape[1]
    onehot = (both_ids[:, :, None] == jnp.arange(expert_count, dtype=jnp.int32)).astype(jnp.int32)
    before = jnp.cumsum(onehot, axis=1) - onehot
    ranks = jnp.sum(before * onehot, axis=2)
    slot_index = both_ids[0] * slot_count + ranks[0]
    origin = jnp.stack([my_half, 1 - my_half])[:, None]
    local_ids = both_ids - my_half * half_count
    target = (local_ids * 2 + origin) * slot_count + ranks
    row_total = expert_count * slot_count
    inside = (local_ids >= 0) & (local_ids < half_count)
    target = jnp.where(inside, target, row_total).reshape(-1)
    source = jnp.full((row_total,), 2 * pair_count, jnp.int32)
    source = source.at[target].set(jnp.arange(2 * pair_count, dtype=jnp.int32), mode="drop")
    empty = jnp.zeros((1, half_width), jnp.bfloat16)
    normed_pad = jnp.concatenate([normed, swap_half(normed), empty], axis=0)
    normed_pad, late_cot = lax.optimization_barrier((normed_pad, layer_cot))
    cot_pad = jnp.concatenate([layer_cot, swap_half(late_cot), empty], axis=0)
    share_pad = jnp.concatenate([both_shares, jnp.zeros((2,), jnp.float32)])
    token_rows = normed_pad[source // 2].reshape(half_count, 2 * slot_count, half_width)
    cot_rows = (cot_pad[source // 2].astype(jnp.float32) * share_pad[source][:, None]).astype(
        jnp.bfloat16
    )
    cot_rows = cot_rows.reshape(half_count, 2 * slot_count, half_width)
    back_rows, grads = expert_pass(token_rows, cot_rows, expert_gate, expert_up, expert_down)
    flat_back = back_rows.reshape(expert_count * slot_count, half_width)
    slots = slot_index.reshape(row_count, 2)
    d_normed = flat_back[slots[:, 0]].astype(jnp.float32) + flat_back[slots[:, 1]].astype(jnp.float32)
    g_dn = gain32 * d_normed
    inner = lax.psum(jnp.sum(mid32 * g_dn, axis=1), "tp") / D
    mid_total = (
        layer_cot.astype(jnp.float32)
        + inv_rms[:, None] * g_dn
        - mid32 * (inv_rms**3 * inner)[:, None]
    )
    mid_grad = mid_total.astype(jnp.bfloat16)
    full_mid = join_pair(mid_grad, 1)
    channel_count = b_gate.shape[1]
    b32 = b_gate.astype(jnp.float32)
    y32 = conv_out.astype(jnp.float32)
    grouped = (b32 * y32).reshape(row_count, channel_count // GROUP, GROUP)
    group_rms = lax.rsqrt(jnp.mean(grouped * grouped, axis=-1) + epsilon)
    cgain = conv_gain.astype(jnp.float32).reshape(channel_count // GROUP, GROUP)
    conv_normed = (
        (grouped * group_rms[..., None] * cgain)
        .reshape(row_count, channel_count)
        .astype(jnp.bfloat16)
    )
    grad_out_weight = scatter_sum(contract_rows(full_mid, conv_normed))
    d_normed_conv = jnp.dot(full_mid, out_weight, preferred_element_type=jnp.float32).reshape(
        grouped.shape
    )
    g_dc = cgain * d_normed_conv
    group_inner = jnp.mean(grouped * g_dc, axis=-1)
    d_gated = (
        group_rms[..., None] * g_dc - grouped * (group_rms**3 * group_inner)[..., None]
    ).reshape(row_count, channel_count)
    grad_b = (d_gated * y32).astype(jnp.bfloat16)
    d_conv_out = d_gated * b32
    following = from_behind(d_conv_out[:2], "sp", -1)
    extended = jnp.concatenate([d_conv_out, following], axis=0)
    taps = conv_taps.astype(jnp.float32)
    d_mixed = taps[2] * extended[:-2] + taps[1] * extended[1:-1] + taps[0] * extended[2:]
    grad_c = (d_mixed * conv_in.astype(jnp.float32)).astype(jnp.bfloat16)
    grad_conv_in = (d_mixed * c_gate.astype(jnp.float32)).astype(jnp.bfloat16)
    return (grads[0], grads[1], grads[2], grad_out_weight, mid_grad, grad_b, grad_c, grad_conv_in)


def solution(mesh):
    placed = (
        P("sp", "tp"),
        P("sp", "tp"),
        P("tp"),
        P("sp", None),
        P("sp"),
        P("sp"),
        P("sp", None, "tp"),
        P("sp", None, "tp"),
        P("sp", "tp", None),
        P(None, "tp"),
        P("tp"),
        P("sp", "tp"),
        P("sp", "tp"),
        P("sp", "tp"),
        P("sp", "tp"),
        P(None, "tp"),
    )
    return jax.shard_map(
        shards,
        mesh=mesh,
        in_specs=placed,
        out_specs=(
            P("sp", None, "tp"),
            P("sp", None, "tp"),
            P("sp", "tp", None),
            P("sp", "tp"),
            P("sp", "tp"),
            P("sp", "tp"),
            P("sp", "tp"),
            P("sp", "tp"),
        ),
        check_vma=False,
    )
```
